32 devices in a mesh: ep: 16 (over z, y, x), tp: 2 (over core).
Axes of the slice: x: 2, y: 2, z: 4, core: 2. Of those that a mesh axis runs over, the one named last changes fastest.
Arguments:
- tokens: bfloat16 [4096, 2048], P('ep'), may hold values from -6 to 6
- expert_ids: int32 [4096, 4], P('ep'), may hold values from 0 to 15, all different within a row; in each aligned block of 256 rows (0 to 255, 256 to 511, ...) at most 96 rows name the same one
- gates: float32 [4096, 4], P('ep'), may hold values from 0.05 to 0.6
- cotangent: bfloat16 [4096, 2048], P('ep'), may hold values from -6 to 6
- w_gate: bfloat16 [16, 2048, 512], P('ep', None, 'tp'), may hold values from -0.125 to 0.125
- w_up: bfloat16 [16, 2048, 512], P('ep', None, 'tp'), may hold values from -0.125 to 0.125
- w_down: bfloat16 [16, 512, 2048], P('ep', 'tp'), may hold values from -0.25 to 0.25
- sh_gate: bfloat16 [2048, 512], P(None, 'tp'), may hold values from -0.125 to 0.125
- sh_up: bfloat16 [2048, 512], P(None, 'tp'), may hold values from -0.125 to 0.125
- sh_down: bfloat16 [512, 2048], P('tp'), may hold values from -0.25 to 0.25
Outputs:
- token_grad: bfloat16 [4096, 2048], P('ep', 'tp')
- gate_grad: float32 [4096, 4], P('ep')
- expert_gate_grad: float32 [16, 2048, 512], P('ep', None, 'tp')
- expert_up_grad: float32 [16, 2048, 512], P('ep', None, 'tp')
- expert_down_grad: float32 [16, 512, 2048], P('ep', 'tp')
- shared_gate_grad: float32 [2048, 512], P('ep', 'tp')
- shared_up_grad: float32 [2048, 512], P('ep', 'tp')
- shared_down_grad: float32 [512, 2048], P('tp', 'ep')
- expert_gate_rows: float32 [16, 2048], P('ep')
- expert_up_rows: float32 [16, 2048], P('ep')
- expert_down_rows: float32 [16, 512], P('ep', 'tp')
- shared_gate_rows: float32 [2048], P('ep')
- shared_up_rows: float32 [2048], P('ep')
- shared_down_rows: float32 [512], P('tp')
The draws below stay inside these ranges and needn't reach their ends.
Inputs may be any that keep to these rules, and one draw needn't show every extreme that they name: `expert_ids`: each row names 4 different experts. Within each aligned block of 256 tokens no expert is named by more than 96 assignments, a bound that is reached in some blocks.
All inputs are finite; a program needn't handle non-finite values.
Results may differ from the reference program's by a relative error of at most 0.0085.
Values may be sent and summed in bfloat16 or wider, within the bound.
A program may use at most 128 MiB of HBM per device.

```python
import math
import jax
import jax.numpy as jnp
import numpy as np
from jax import lax

D = 2048
HID = 512
SH = 512
TOP_K = 4
TOK_DEV = 256
EXPERTS = 16
CAP = 96
TOKENS = 4096
N_TP = 2


def with_spikes(values, stream_key, source, target, parts, factor):
    def block_of(position):
        return (jnp.arange(values.shape[position]) // (values.shape[position] // parts)).reshape((-1,) + (1,) * (values.ndim - 1 - position))

    first = jax.random.permutation(stream_key, parts)[block_of(target)]
    second = (block_of(target) + parts // 2) % parts
    return jnp.where((block_of(source) == first) | (block_of(source) == second), factor * values, values)


def levels(stream_key, shape, split, least, high):
    def one(dim, shards_of):
        steps = jax.random.uniform(jax.random.fold_in(jax.random.fold_in(stream_key, 6), dim), (shards_of,), jnp.float32, least / len(split), high / len(split))
        return jnp.repeat(jnp.exp(steps), shape[dim] // shards_of).reshape((-1,) + (1,) * (len(shape) - dim - 1))

    loudness = one(*split[0])
    for cut in split[1:]:
        loudness = loudness * one(*cut)
    return loudness


def deal_out(stream_key, own, number, rows, amount, top, reach, skew):
    ranking = jax.random.permutation(stream_key, amount)
    crowded, ordinary = load_shares(amount, rows * top, reach, skew, True), load_shares(amount, rows * top, reach, skew, False)
    places = jnp.arange(amount)

    def named(sizes, offset_by):
        used = int((sizes > 0).sum())
        fixed = max(1, used // 4)
        passed = fixed + (places - fixed + offset_by * (used - fixed)) % max(1, amount - fixed)
        return jnp.zeros((amount,), jnp.int32).at[ranking[jnp.where(places < fixed, places, passed)]].set(jnp.asarray(sizes, jnp.int32))

    sizes = jnp.where(number % 4 == 0, named(crowded, number // 4), named(ordinary, number - number // 4 - 1))
    mixed = jax.random.permutation(jax.random.fold_in(own, 3), amount)
    giver, sink = mixed[0:amount // 2 * 2:2], mixed[1:amount // 2 * 2:2]
    room = jnp.minimum(sizes[giver] - 1, reach - sizes[sink]) // 2
    room = jnp.where((giver == ranking[0]) | (sink == ranking[0]) | (sizes[sink] == 0), 0, jnp.maximum(room, 0))
    passed = jax.random.randint(jax.random.fold_in(own, 4), (amount // 2,), 0, 1 << 20) % (room + 1)
    sizes = sizes.at[giver].add(-passed).at[sink].add(passed)
    members = jnp.searchsorted(jnp.cumsum(sizes), jnp.arange(rows * top), side="right").astype(jnp.int32)
    grid = members.reshape(top, rows).T
    grid = grid[jax.random.permutation(jax.random.fold_in(own, 1), rows)]
    offset_by = jax.random.randint(jax.random.fold_in(own, 2), (rows, 1), 0, top)
    return jnp.take_along_axis(grid, (jnp.arange(top)[None, :] + offset_by) % top, axis=1)


def load_shares(count, total, most, skew, full):
    weights = [(1 << 20) // math.isqrt(grade ** skew) + 1 for grade in range(1, count + 1)]
    largest = most if full else min(most, max(-(-total // count), total * weights[0] // sum(weights)))
    least = 1 if total - largest >= count - 1 else 0
    given, spare = [largest] + [least] * (count - 1), total - largest - least * (count - 1)
    while spare > 0:
        movable = [i for i in range(1, count) if given[i] < largest] or [i for i in range(1, count) if given[i] < most]
        mass, remaining = sum([weights[i] for i in movable]), spare
        for i in movable:
            addition = min(most - given[i], max(1, remaining * weights[i] // mass), spare)
            given[i] = given[i] + addition
            spare = spare - addition
    return np.array(given)


def bell_draw(key, shape, deviation, reach, shards=(), kind=jnp.bfloat16):
    array = deviation * jax.random.normal(key, shape, jnp.float32)
    if shards:
        array = array * levels(key, shape, shards, -0.22, 0.18)
    return jnp.clip(array, -reach, reach).astype(kind)


def noise_with(key, extent, deviation, bound, cuts, heavy, kind=jnp.bfloat16):
    values = deviation * jax.random.normal(key, extent, jnp.float32)
    if cuts:
        values = values * levels(key, extent, cuts, -0.22, 0.18)
    return jnp.clip(with_spikes(values, jax.random.fold_in(key, 3), *heavy), -bound, bound).astype(kind)


def setup_inputs(seed: int = 0) -> dict:
    keys = jax.random.split(jax.random.key(seed), 11)
    tokens = noise_with(keys[0], (TOKENS, D), 1.0, 6.0, ((0, 16),), (0, 1, 16, 2.0))
    expert_ids_keys = jax.random.split(jax.random.fold_in(keys[1], 1), TOKENS // TOK_DEV)
    expert_ids_turns = jax.random.permutation(jax.random.fold_in(keys[1], 3), TOKENS // TOK_DEV)
    expert_ids = jax.vmap(lambda own, number: deal_out(jax.random.fold_in(keys[1], 2), own, number, TOK_DEV, EXPERTS, TOP_K, CAP, 2))(expert_ids_keys, expert_ids_turns).reshape((TOKENS, TOP_K))
    gates = jnp.clip(0.05 + 0.55 * jax.random.uniform(keys[2], (TOKENS, TOP_K), jnp.float32) ** levels(keys[2], (TOKENS, TOP_K), ((0, 16),), -0.2, 0.2), 0.05, 0.6)
    cotangent = noise_with(keys[3], (TOKENS, D), 1.0, 6.0, ((0, 16),), (0, 1, 16, 2.0))
    w_gate = bell_draw(keys[4], (EXPERTS, D, HID), D ** -0.5, 0.125, ((0, 16), (2, 2)))
    w_up = bell_draw(keys[5], (EXPERTS, D, HID), D ** -0.5, 0.125, ((0, 16), (2, 2)))
    w_down = bell_draw(keys[6], (EXPERTS, HID, D), HID ** -0.5, 0.25, ((0, 16), (1, 2)))
    sh_gate = bell_draw(keys[7], (D, SH), D ** -0.5, 0.125, ((1, 2),))
    sh_up = bell_draw(keys[8], (D, SH), D ** -0.5, 0.125, ((1, 2),))
    sh_down = bell_draw(keys[9], (SH, D), SH ** -0.5, 0.25, ((0, 2),))
    return dict(tokens=tokens, expert_ids=expert_ids, gates=gates, cotangent=cotangent, w_gate=w_gate, w_up=w_up, w_down=w_down, sh_gate=sh_gate, sh_up=sh_up, sh_down=sh_down)


def silu_parts(pre):
    sigmoid = jax.nn.sigmoid(pre)
    return pre * sigmoid, sigmoid * (1.0 + pre * (1.0 - sigmoid))


def halves_sum(left_a, right_a, left_b, right_b, pieces):
    step_cols = left_a.shape[1] // pieces
    total = jnp.zeros((left_a.shape[0], right_a.shape[0]), jnp.float32)
    for piece in range(pieces):
        first_col = piece * step_cols
        part = jnp.dot(left_a[:, first_col:first_col + step_cols], right_a[:, first_col:first_col + step_cols].T, preferred_element_type=jnp.float32)
        part = part + jnp.dot(left_b[:, first_col:first_col + step_cols], right_b[:, first_col:first_col + step_cols].T, preferred_element_type=jnp.float32)
        total = total + lax.optimization_barrier(part.astype(jnp.bfloat16)).astype(jnp.float32)
    return total


def backward_rows(inputs, cot_rows, w_g, w_u, w_d):
    gate_pre = jnp.dot(inputs, w_g, preferred_element_type=jnp.float32)
    up_pre = jnp.dot(inputs, w_u, preferred_element_type=jnp.float32)
    active, slope = silu_parts(gate_pre)
    hidden = (active * up_pre).astype(jnp.bfloat16)
    hidden_cot = jnp.dot(cot_rows, w_d.T, preferred_element_type=jnp.float32)
    gate_sum = jnp.sum(hidden.astype(jnp.float32) * hidden_cot, axis=1)
    d_gate = (hidden_cot * up_pre * slope).astype(jnp.bfloat16)
    d_up = (hidden_cot * active).astype(jnp.bfloat16)
    grad_g = jnp.dot(inputs.T, d_gate, preferred_element_type=jnp.float32)
    grad_u = jnp.dot(inputs.T, d_up, preferred_element_type=jnp.float32)
    grad_d = jnp.dot(hidden.T, cot_rows, preferred_element_type=jnp.float32)
    rows = halves_sum(d_gate, w_g, d_up, w_u, N_TP)
    return grad_g, grad_u, grad_d, rows, gate_sum


def reference(tokens, expert_ids, gates, cotangent, w_gate, w_up, w_down, sh_gate, sh_up, sh_down):
    per_dev = TOK_DEV * TOP_K
    assign = TOKENS * TOP_K
    slots = EXPERTS * CAP
    flat_ids = expert_ids.reshape(EXPERTS, per_dev).astype(jnp.int32)
    onehot = (flat_ids[:, :, None] == jnp.arange(EXPERTS, dtype=jnp.int32)[None, None, :]).astype(jnp.int32)
    slot_rank = jnp.sum((jnp.cumsum(onehot, axis=1) - 1) * onehot, axis=2)
    sources = jnp.arange(EXPERTS, dtype=jnp.int32)[:, None]
    slot_row = (flat_ids * slots + sources * CAP + slot_rank).reshape(assign).astype(jnp.int32)
    slot_table = jnp.full((EXPERTS * slots,), assign, jnp.int32).at[slot_row].set(jnp.arange(assign, dtype=jnp.int32))
    filled = slot_table < assign
    source = jnp.minimum(slot_table, assign - 1)
    token_row = (source // TOP_K).astype(jnp.int32)
    slot_gate = jnp.where(filled, gates.reshape(assign)[source], jnp.zeros((), jnp.float32))

    def one_expert(packed):
        rows_index, gate_col, keep, w_g, w_u, w_d = packed
        inputs = jnp.where(keep[:, None], tokens[rows_index], jnp.zeros((), tokens.dtype))
        cot_rows = (gate_col[:, None] * cotangent[rows_index].astype(jnp.float32)).astype(jnp.bfloat16)
        return backward_rows(inputs, cot_rows, w_g, w_u, w_d)

    grad_g, grad_u, grad_d, slot_rows, gate_sums = lax.map(one_expert, (token_row.reshape(EXPERTS, slots), slot_gate.reshape(EXPERTS, slots), filled.reshape(EXPERTS, slots), w_gate, w_up, w_down))
    flat_rows = slot_rows.reshape(EXPERTS * slots, D)
    picks = slot_row.reshape(TOKENS, TOP_K)
    routed = jnp.zeros((TOKENS, D), jnp.float32)
    for column in range(TOP_K):
        routed = routed + flat_rows[picks[:, column]].astype(jnp.float32)
    gate_grad = gate_sums.reshape(EXPERTS * slots)[picks] / gates
    shared_g, shared_u, shared_d, shared_rows, unused = backward_rows(tokens, cotangent, sh_gate, sh_up, sh_down)
    token_grad = (routed + shared_rows).astype(jnp.bfloat16)
    return (token_grad, gate_grad, grad_g, grad_u, grad_d, shared_g, shared_u, shared_d,
            jnp.sum(grad_g * grad_g, axis=2), jnp.sum(grad_u * grad_u, axis=2), jnp.sum(grad_d * grad_d, axis=2),
            jnp.sum(shared_g * shared_g, axis=1), jnp.sum(shared_u * shared_u, axis=1), jnp.sum(shared_d * shared_d, axis=1))
```

```python
import functools
import math

import jax
import jax.numpy as jnp
from jax import lax
from jax.experimental import pallas as pl
from jax.experimental.pallas import tpu as pltpu
from jax.sharding import PartitionSpec as P

BF16 = jnp.bfloat16
F32 = jnp.float32


def silu_parts(pre):
    sigmoid = jax.nn.sigmoid(pre)
    return (pre * sigmoid, sigmoid * (1.0 + pre * (1.0 - sigmoid)))


def expert_backward(inputs, cot_rows, w_g, w_u, w_d):
    gate_pre = jnp.dot(inputs, w_g, preferred_element_type=F32)
    up_pre = jnp.dot(inputs, w_u, preferred_element_type=F32)
    active, slope = silu_parts(gate_pre)
    hidden = (active * up_pre).astype(BF16)
    hidden_cot = jnp.dot(cot_rows, w_d.T, preferred_element_type=F32)
    gate_part = jnp.sum(hidden.astype(F32) * hidden_cot, axis=1)
    d_gate = (hidden_cot * up_pre * slope).astype(BF16)
    d_up = (hidden_cot * active).astype(BF16)
    contract = (((0,), (0,)), ((), ()))
    grad_g = lax.dot_general(inputs, d_gate, contract, preferred_element_type=F32)
    grad_u = lax.dot_general(inputs, d_up, contract, preferred_element_type=F32)
    grad_d = lax.dot_general(hidden, cot_rows, contract, preferred_element_type=F32)
    partial_value = jnp.dot(d_gate, w_g.T, preferred_element_type=F32) + jnp.dot(
        d_up, w_u.T, preferred_element_type=F32
    )
    return (grad_g, grad_u, grad_d, partial_value.astype(BF16), gate_part)


def plane_count(mesh):
    count = mesh.shape["ep"]
    try:
        planes = len({tuple(d.coords)[2] for d in mesh.devices.flat})
    except (AttributeError, TypeError, IndexError):
        planes = 0
    if planes < 1 or count % planes:
        planes = max(d for d in range(1, math.isqrt(count) + 1) if count % d == 0)
    return planes


def copy_to(src, dst, send, recv, ep, tp):
    return pltpu.make_async_remote_copy(
        src_ref=src,
        dst_ref=dst,
        send_sem=send,
        recv_sem=recv,
        device_id=(ep, tp),
        device_id_type=pl.DeviceIdType.MESH,
    )


def combine_kernel(
    planes, width,
    own, oth, sh_own, sh_oth, scatter, grads,
    tok_out, grad_out,
    tp_in, sh_in, sums, plane_in, gplane_in, z_out, z_in, gz_out, gz_in, routed, gtotal,
    tp_sem, plane_sem, gplane_sem, z_sem, gz_sem,
):
    me, core = lax.axis_index("ep"), lax.axis_index("tp")
    z, q = me // width, me % width
    order = list(range(1, planes)) + [0]
    dest_z = [(z + step) % planes for step in order]
    dest_q = [(q + step) % width for step in range(width)]
    started = []

    def start(copy):
        copy.start()
        started.append(copy)
        return copy

    tp_copies = [
        start(copy_to(oth.at[dest_z[i]], tp_in.at[i], tp_sem.at[0, i], tp_sem.at[1, i], me, 1 - core))
        for i in range(planes)
    ]
    sh_copy = start(
        copy_to(sh_oth, sh_in, tp_sem.at[0, planes], tp_sem.at[1, planes], me, 1 - core)
    )
    plane_copies, gplane_copies = {}, {}
    for i in range(planes):
        for d in range(1, width):
            peer = z * width + dest_q[d]
            gplane_copies[i, d] = start(
                copy_to(
                    grads.at[dest_z[i], dest_q[d]],
                    gplane_in.at[i, d - 1],
                    gplane_sem.at[0, i, d - 1],
                    gplane_sem.at[1, i, d - 1],
                    peer,
                    core,
                )
            )
        tp_copies[i].wait_recv()
        for d in range(width):
            sums[i, d] = (
                own[dest_z[i], dest_q[d]].astype(F32) + tp_in[i, dest_q[d]].astype(F32)
            ).astype(BF16)
            if d:
                peer = z * width + dest_q[d]
                plane_copies[i, d] = start(
                    copy_to(
                        sums.at[i, d],
                        plane_in.at[i, d - 1],
                        plane_sem.at[0, i, d - 1],
                        plane_sem.at[1, i, d - 1],
                        peer,
                        core,
                    )
                )
    z_copies = []
    for i in range(planes):
        peer = dest_z[i] * width + q
        total = grads[dest_z[i], q].astype(F32)
        for d in range(1, width):
            gplane_copies[i, d].wait_recv()
            total = total + gplane_in[i, d - 1].astype(F32)
        if i < planes - 1:
            gz_out[i] = total.astype(BF16)
            z_copies.append(
                start(copy_to(gz_out.at[i], gz_in.at[i], gz_sem.at[0, i], gz_sem.at[1, i], peer, core))
            )
        else:
            gtotal[...] = total
        for d in range(1, width):
            plane_copies[i, d].wait_recv()
        acc = jnp.dot(scatter[dest_z[i], 0], sums[i, 0], preferred_element_type=F32)
        for d in range(1, width):
            acc = acc + jnp.dot(
                scatter[dest_z[i], d], plane_in[i, d - 1], preferred_element_type=F32
            )
        if i < planes - 1:
            z_out[i] = acc.astype(BF16)
            z_copies.append(
                start(copy_to(z_out.at[i], z_in.at[i], z_sem.at[0, i], z_sem.at[1, i], peer, core))
            )
        else:
            routed[...] = acc
    sh_copy.wait_recv()
    for copy in z_copies:
        copy.wait_recv()
    total = gtotal[...]
    acc = routed[...]
    for i in range(planes - 1):
        total = total + gz_in[i].astype(F32)
        acc = acc + z_in[i].astype(F32)
    grad_out[...] = total
    acc = acc + (sh_own[...].astype(F32) + sh_in[...].astype(F32))
    tok_out[...] = acc.astype(BF16)
    for copy in started:
        copy.wait_send()


def combine(planes, own, oth, sh_own, sh_oth, scatter, grads):
    width = own.shape[1]
    cap, cols = own.shape[2:]
    rows = sh_own.shape[0]
    g_shape = grads.shape[2:]
    vmem = pl.BlockSpec(memory_space=pltpu.VMEM)
    far, side = max(planes - 1, 1), max(width - 1, 1)
    return pl.pallas_call(
        functools.partial(combine_kernel, planes, width),
        out_shape=(
            jax.ShapeDtypeStruct((rows, cols), BF16),
            jax.ShapeDtypeStruct(g_shape, F32),
        ),
        in_specs=[vmem] * 6,
        out_specs=(vmem, vmem),
        scratch_shapes=[
            pltpu.VMEM((planes, width, cap, cols), BF16),
            pltpu.VMEM((rows, cols), BF16),
            pltpu.VMEM((planes, width, cap, cols), BF16),
            pltpu.VMEM((planes, side, cap, cols), BF16),
            pltpu.VMEM((planes, side) + g_shape, BF16),
            pltpu.VMEM((far, rows, cols), BF16),
            pltpu.VMEM((far, rows, cols), BF16),
            pltpu.VMEM((far,) + g_shape, BF16),
            pltpu.VMEM((far,) + g_shape, BF16),
            pltpu.VMEM((rows, cols), F32),
            pltpu.VMEM(g_shape, F32),
            pltpu.SemaphoreType.DMA((2, planes + 1)),
            pltpu.SemaphoreType.DMA((2, planes, side)),
            pltpu.SemaphoreType.DMA((2, planes, side)),
            pltpu.SemaphoreType.DMA((2, far)),
            pltpu.SemaphoreType.DMA((2, far)),
        ],
        compiler_params=pltpu.CompilerParams(
            has_side_effects=True, vmem_limit_bytes=60 * 2**20
        ),
        name="combine",
    )(own, oth, sh_own, sh_oth, scatter, grads)


def local(planes, tokens, expert_ids, gates, cotangent, w_gate, w_up, w_down, sh_gate, sh_up, sh_down):
    experts_count = lax.axis_size("ep")
    width = experts_count // planes
    me, core = lax.axis_index("ep"), lax.axis_index("tp")
    z, q = me // width, me % width
    tok_rows, model_width = tokens.shape
    top_count = expert_ids.shape[1]
    capacity = 3 * tok_rows * top_count // (2 * experts_count)
    half_cols = model_width // lax.axis_size("tp")
    first_col = core * half_cols

    all_ids = lax.all_gather(expert_ids, "ep", axis=0)
    line_ids = lax.dynamic_index_in_dim(
        all_ids.reshape(planes, width, tok_rows, top_count), q, 1, keepdims=False
    )
    lanes = jnp.arange(experts_count, dtype=jnp.int32)
    earlier = jnp.tril(jnp.ones((tok_rows, tok_rows), BF16), -1)

    def ranks_of(names):
        rank = jnp.dot(earlier, names.astype(BF16), preferred_element_type=F32)
        return jnp.where(names, rank.astype(jnp.int32), -1)

    mine = expert_ids[:, :, None] == lanes
    rank = ranks_of(jnp.any(mine, axis=1))
    gate_of = jnp.sum(jnp.where(mine, gates[:, :, None], 0.0), axis=1)
    slots = jnp.arange(capacity, dtype=jnp.int32)
    picked = rank.T[:, None, :] == slots[None, :, None]
    slot_gate = jnp.sum(jnp.where(picked, gate_of.T[:, None, :], 0.0), axis=2)
    picked_rows = picked.astype(BF16).reshape(experts_count * capacity, tok_rows)

    tok_half = lax.dynamic_slice_in_dim(tokens, first_col, half_cols, 1)
    cot_half = lax.dynamic_slice_in_dim(cotangent, first_col, half_cols, 1)
    inputs = jnp.dot(picked_rows, tok_half, preferred_element_type=F32).astype(BF16)
    scaled = (
        jnp.dot(picked_rows, cot_half, preferred_element_type=F32) * slot_gate.reshape(-1, 1)
    ).astype(BF16)
    part_in, part_cot = (
        lax.all_to_all(inputs, "ep", split_axis=0, concat_axis=0, tiled=True),
        lax.all_to_all(scaled, "ep", split_axis=0, concat_axis=0, tiled=True),
    )
    got_in, got_cot = (
        lax.all_gather(part_in, "tp", axis=1, tiled=True),
        lax.all_gather(part_cot, "tp", axis=1, tiled=True),
    )
    shared_g, shared_u, shared_d, shared_part, unused = expert_backward(
        tokens, cotangent, sh_gate, sh_up, sh_down
    )
    grad_g, grad_u, grad_d, routed_part, gate_part = expert_backward(
        got_in, got_cot, w_gate[0], w_up[0], w_down[0]
    )

    part_rows = model_width // experts_count
    hidden_cols = sh_gate.shape[1]
    pieces = hidden_cols // part_rows
    deal = (planes, width, part_rows, hidden_cols)
    down = shared_d.astype(BF16).reshape(pieces, part_rows, experts_count, part_rows)
    down = down.transpose(2, 1, 0, 3).reshape(deal)
    grads = jnp.concatenate(
        [shared_g.astype(BF16).reshape(deal), shared_u.astype(BF16).reshape(deal), down], axis=2
    )

    senders = z * width + (q - jnp.arange(width, dtype=jnp.int32)) % width
    named = line_ids[:, :, :, None] == senders
    named = jnp.any(named, axis=2)
    line_rank = jax.vmap(ranks_of)(named)
    scatter = (line_rank.transpose(0, 2, 1)[..., None] == slots).astype(BF16)

    def halves(values):
        return (
            lax.dynamic_slice_in_dim(values, first_col, half_cols, 1),
            lax.dynamic_slice_in_dim(values, half_cols - first_col, half_cols, 1),
        )

    own, oth = halves(routed_part)
    sh_own, sh_oth = halves(shared_part)
    blocks = (planes, width, capacity, half_cols)
    token_grad, shared_sum = combine(
        planes, own.reshape(blocks), oth.reshape(blocks), sh_own, sh_oth, scatter, grads
    )
    out_g = shared_sum[:part_rows]
    out_u = shared_sum[part_rows : 2 * part_rows]
    out_d = (
        shared_sum[2 * part_rows :]
        .reshape(part_rows, pieces, part_rows)
        .transpose(1, 0, 2)
        .reshape(hidden_cols, part_rows)
    )

    down_part = jnp.sum(out_d * out_d, axis=1)
    small = jnp.concatenate(
        [
            gate_part.reshape(experts_count, capacity),
            jnp.broadcast_to(down_part, (experts_count, hidden_cols)),
        ],
        axis=1,
    )
    small = lax.all_to_all(small, "ep", split_axis=0, concat_axis=0, tiled=True)
    back_gate, gate_norms, up_norms, shared_gate_norms, shared_up_norms = lax.psum(
        (
            small[:, :capacity],
            jnp.sum(grad_g * grad_g, axis=1),
            jnp.sum(grad_u * grad_u, axis=1),
            jnp.sum(out_g * out_g, axis=1),
            jnp.sum(out_u * out_u, axis=1),
        ),
        "tp",
    )
    down_norms = jnp.sum(small[:, capacity:], axis=0)
    token_gate = jnp.sum(jnp.where(picked, back_gate[:, :, None], 0.0), axis=1)
    gate_grad = jnp.sum(jnp.where(mine, token_gate.T[:, None, :], 0.0), axis=2) / gates
    return (
        token_grad,
        gate_grad,
        grad_g[None],
        grad_u[None],
        grad_d[None],
        out_g,
        out_u,
        out_d,
        gate_norms[None],
        up_norms[None],
        jnp.sum(grad_d * grad_d, axis=1)[None],
        shared_gate_norms,
        shared_up_norms,
        down_norms,
    )


def solution(mesh):
    placed = (
        P("ep", None),
        P("ep", None),
        P("ep", None),
        P("ep", None),
        P("ep", None, "tp"),
        P("ep", None, "tp"),
        P("ep", "tp", None),
        P(None, "tp"),
        P(None, "tp"),
        P("tp", None),
    )
    return jax.shard_map(
        functools.partial(local, plane_count(mesh)),
        mesh=mesh,
        in_specs=placed,
        out_specs=(
            P("ep", "tp"),
            P("ep", None),
            P("ep", None, "tp"),
            P("ep", None, "tp"),
            P("ep", "tp", None),
            P("ep", "tp"),
            P("ep", "tp"),
            P("tp", "ep"),
            P("ep", None),
            P("ep", None),
            P("ep", "tp"),
            P("ep"),
            P("ep"),
            P("tp"),
        ),
        check_vma=False,
    )
```

```python
import functools
import math

import jax
import jax.numpy as jnp
from jax import lax
from jax.experimental import pallas as pl
from jax.experimental.pallas import tpu as pltpu
from jax.sharding import PartitionSpec as P

BF16 = jnp.bfloat16
F32 = jnp.float32


def silu_parts(pre):
    sigmoid = jax.nn.sigmoid(pre)
    return (pre * sigmoid, sigmoid * (1.0 + pre * (1.0 - sigmoid)))


def expert_backward(inputs, cot_rows, w_g, w_u, w_d):
    gate_pre = jnp.dot(inputs, w_g, preferred_element_type=F32)
    up_pre = jnp.dot(inputs, w_u, preferred_element_type=F32)
    active, slope = silu_parts(gate_pre)
    hidden = (active * up_pre).astype(BF16)
    hidden_cot = jnp.dot(cot_rows, w_d.T, preferred_element_type=F32)
    gate_part = jnp.sum(hidden.astype(F32) * hidden_cot, axis=1)
    d_gate = (hidden_cot * up_pre * slope).astype(BF16)
    d_up = (hidden_cot * active).astype(BF16)
    contract = (((0,), (0,)), ((), ()))
    grad_g = lax.dot_general(inputs, d_gate, contract, preferred_element_type=F32)
    grad_u = lax.dot_general(inputs, d_up, contract, preferred_element_type=F32)
    grad_d = lax.dot_general(hidden, cot_rows, contract, preferred_element_type=F32)
    partial_value = jnp.dot(d_gate, w_g.T, preferred_element_type=F32) + jnp.dot(
        d_up, w_u.T, preferred_element_type=F32
    )
    return (grad_g, grad_u, grad_d, partial_value.astype(BF16), gate_part)


def plane_count(mesh):
    count = mesh.shape["ep"]
    try:
        planes = len({tuple(d.coords)[2] for d in mesh.devices.flat})
    except (AttributeError, TypeError, IndexError):
        planes = 0
    if planes < 1 or count % planes:
        planes = max(d for d in range(1, math.isqrt(count) + 1) if count % d == 0)
    return planes


def copy_to(src, dst, send, recv, ep, tp):
    return pltpu.make_async_remote_copy(
        src_ref=src,
        dst_ref=dst,
        send_sem=send,
        recv_sem=recv,
        device_id=(ep, tp),
        device_id_type=pl.DeviceIdType.MESH,
    )


def combine_kernel(
    planes, width,
    own, oth, sh_own, sh_oth, scatter, grads,
    tok_out, grad_out,
    tp_in, sh_in, sums, plane_in, gplane_in, z_out, z_in, gz_out, gz_in, routed, gtotal,
    tp_sem, plane_sem, gplane_sem, z_sem, gz_sem,
):
    me, core = lax.axis_index("ep"), lax.axis_index("tp")
    z, q = me // width, me % width
    order = list(range(1, planes)) + [0]
    dest_z = [(z + step) % planes for step in order]
    dest_q = [(q + step) % width for step in range(width)]
    started = []

    def start(copy):
        copy.start()
        started.append(copy)
        return copy

    tp_copies = [
        start(copy_to(oth.at[dest_z[i]], tp_in.at[i], tp_sem.at[0, i], tp_sem.at[1, i], me, 1 - core))
        for i in range(planes)
    ]
    sh_copy = start(
        copy_to(sh_oth, sh_in, tp_sem.at[0, planes], tp_sem.at[1, planes], me, 1 - core)
    )
    plane_copies, gplane_copies = {}, {}
    for i in range(planes):
        for d in range(1, width):
            peer = z * width + dest_q[d]
            gplane_copies[i, d] = start(
                copy_to(
                    grads.at[dest_z[i], dest_q[d]],
                    gplane_in.at[i, d - 1],
                    gplane_sem.at[0, i, d - 1],
                    gplane_sem.at[1, i, d - 1],
                    peer,
                    core,
                )
            )
        tp_copies[i].wait_recv()
        for d in range(width):
            sums[i, d] = (
                own[dest_z[i], dest_q[d]].astype(F32) + tp_in[i, dest_q[d]].astype(F32)
            ).astype(BF16)
            if d:
                peer = z * width + dest_q[d]
                plane_copies[i, d] = start(
                    copy_to(
                        sums.at[i, d],
                        plane_in.at[i, d - 1],
                        plane_sem.at[0, i, d - 1],
                        plane_sem.at[1, i, d - 1],
                        peer,
                        core,
                    )
                )
    z_copies = []
    for i in range(planes):
        peer = dest_z[i] * width + q
        total = grads[dest_z[i], q].astype(F32)
        for d in range(1, width):
            gplane_copies[i, d].wait_recv()
            total = total + gplane_in[i, d - 1].astype(F32)
        if i < planes - 1:
            gz_out[i] = total.astype(BF16)
            z_copies.append(
                start(copy_to(gz_out.at[i], gz_in.at[i], gz_sem.at[0, i], gz_sem.at[1, i], peer, core))
            )
        else:
            gtotal[...] = total
        for d in range(1, width):
            plane_copies[i, d].wait_recv()
        acc = jnp.dot(scatter[dest_z[i], 0], sums[i, 0], preferred_element_type=F32)
        for d in range(1, width):
            acc = acc + jnp.dot(
                scatter[dest_z[i], d], plane_in[i, d - 1], preferred_element_type=F32
            )
        if i < planes - 1:
            z_out[i] = acc.astype(BF16)
            z_copies.append(
                start(copy_to(z_out.at[i], z_in.at[i], z_sem.at[0, i], z_sem.at[1, i], peer, core))
            )
        else:
            routed[...] = acc
    sh_copy.wait_recv()
    for copy in z_copies:
        copy.wait_recv()
    total = gtotal[...]
    acc = routed[...]
    for i in range(planes - 1):
        total = total + gz_in[i].astype(F32)
        acc = acc + z_in[i].astype(F32)
    grad_out[...] = total
    acc = acc + (sh_own[...].astype(F32) + sh_in[...].astype(F32))
    tok_out[...] = acc.astype(BF16)
    for copy in started:
        copy.wait_send()


def combine(planes, own, oth, sh_own, sh_oth, scatter, grads):
    width = own.shape[1]
    cap, cols = own.shape[2:]
    rows = sh_own.shape[0]
    g_shape = grads.shape[2:]
    vmem = pl.BlockSpec(memory_space=pltpu.VMEM)
    far, side = max(planes - 1, 1), max(width - 1, 1)
    return pl.pallas_call(
        functools.partial(combine_kernel, planes, width),
        out_shape=(
            jax.ShapeDtypeStruct((rows, cols), BF16),
            jax.ShapeDtypeStruct(g_shape, F32),
        ),
        in_specs=[vmem] * 6,
        out_specs=(vmem, vmem),
        scratch_shapes=[
            pltpu.VMEM((planes, width, cap, cols), BF16),
            pltpu.VMEM((rows, cols), BF16),
            pltpu.VMEM((planes, width, cap, cols), BF16),
            pltpu.VMEM((planes, side, cap, cols), BF16),
            pltpu.VMEM((planes, side) + g_shape, BF16),
            pltpu.VMEM((far, rows, cols), BF16),
            pltpu.VMEM((far, rows, cols), BF16),
            pltpu.VMEM((far,) + g_shape, BF16),
            pltpu.VMEM((far,) + g_shape, BF16),
            pltpu.VMEM((rows, cols), F32),
            pltpu.VMEM(g_shape, F32),
            pltpu.SemaphoreType.DMA((2, planes + 1)),
            pltpu.SemaphoreType.DMA((2, planes, side)),
            pltpu.SemaphoreType.DMA((2, planes, side)),
            pltpu.SemaphoreType.DMA((2, far)),
            pltpu.SemaphoreType.DMA((2, far)),
        ],
        compiler_params=pltpu.CompilerParams(
            has_side_effects=True, vmem_limit_bytes=60 * 2**20
        ),
        name="combine",
    )(own, oth, sh_own, sh_oth, scatter, grads)


def dispatch_kernel(
    planes, width, cap,
    x, table,
    tok_out, cot_out, line_table,
    held, ready,
    table_sem, line_sem, plane_sem, own_sem, pair_sem,
):
    me, core = lax.axis_index("ep"), lax.axis_index("tp")
    z, q = me // width, me % width
    cols = x.shape[1] // 2
    mine = pl.ds(pl.multiple_of(core * cols, cols), cols)
    outs = (tok_out, cot_out)

    table_copies = []
    for step in range(1, planes):
        peer = (z + step) % planes * width + q
        copy = copy_to(
            table, line_table.at[z], table_sem.at[0, step - 1], table_sem.at[1, step - 1], peer, core
        )
        copy.start()
        table_copies.append(copy)
    line_table[z] = table[...]

    def hop(step, way):
        block = z - (step - 1) if way == 0 else z + (step - 1)
        there = z + 1 if way == 0 else z - 1
        valid = (block >= 0) & (block < planes) & (there >= 0) & (there < planes)
        block, there = jnp.clip(block, 0, planes - 1), jnp.clip(there, 0, planes - 1)
        source = x if step == 1 else held.at[block]
        copy = copy_to(
            source,
            held.at[block],
            line_sem.at[0, step - 1, way],
            line_sem.at[1, step - 1, way],
            there * width + q,
            core,
        )
        return valid, copy

    def arrival(step, way):
        block = z - step if way == 0 else z + step
        valid = (block >= 0) & (block < planes)
        block = jnp.clip(block, 0, planes - 1)
        copy = copy_to(
            held.at[block],
            held.at[block],
            line_sem.at[0, step - 1, way],
            line_sem.at[1, step - 1, way],
            me,
            1 - core,
        )
        return valid, block, copy

    def send_step(step):
        for way in range(2):
            valid, copy = hop(step, way)

            @pl.when(valid)
            def _(copy=copy):
                copy.start()

    def plane_copy(block, d, part, from_q, to_q):
        return copy_to(
            ready.at[block, d, :, pl.ds(part * cols, cols)],
            outs[part].at[block, from_q, :, mine],
            plane_sem.at[0, block, d, part],
            plane_sem.at[1, block, d, part],
            z * width + to_q,
            core,
        )

    def own_copy(block, part):
        return pltpu.make_async_copy(
            ready.at[block, 0, :, pl.ds(part * cols, cols)],
            outs[part].at[block, q, :, mine],
            own_sem.at[block, part],
        )

    def pair_copy(block, d, part):
        from_q = (q + width - d) % width
        return copy_to(
            outs[part].at[block, from_q, :, mine],
            outs[part].at[block, from_q, :, mine],
            pair_sem.at[0, block, d, part],
            pair_sem.at[1, block, d, part],
            me,
            1 - core,
        )

    def select(block, source):
        def one(index, carry):
            d = (index + 1) % width
            to_q = (q + d) % width
            expert = z * width + to_q
            ranks = line_table[block, 0, pl.ds(expert, 1), :]
            gates = line_table[block, 1, pl.ds(expert, 1), :]
            slots = lax.broadcasted_iota(jnp.int32, (cap, ranks.shape[1]), 0).astype(F32)
            hit = slots == ranks
            gate = jnp.sum(jnp.where(hit, gates, 0.0), axis=1, keepdims=True)
            rows = jnp.dot(
                jnp.where(hit, 1.0, 0.0).astype(BF16), source[...], preferred_element_type=F32
            )
            ready[block, d, :, :cols] = rows[:, :cols].astype(BF16)
            ready[block, d, :, cols:] = (rows[:, cols:] * gate).astype(BF16)

            @pl.when(d > 0)
            def _():
                for part in range(2):
                    plane_copy(block, d, part, q, to_q).start()

            @pl.when(d == 0)
            def _():
                for part in range(2):
                    own_copy(block, part).start()

            return carry

        lax.fori_loop(0, width, one, 0)

    def pass_on(block):
        for part in range(2):
            own_copy(block, part).wait()
            pair_copy(block, 0, part).start()

        def one(d, carry):
            for part in range(2):
                plane_copy(block, d, part, (q + width - d) % width, (q + d) % width).wait_recv()
                pair_copy(block, d, part).start()
            return carry

        lax.fori_loop(1, width, one, 0)

    send_step(1)
    select(z, x)
    for copy in table_copies:
        copy.wait_recv()
    for step in range(1, planes):
        for way in range(2):
            valid, block, copy = arrival(step, way)

            @pl.when(valid)
            def _(copy=copy):
                copy.wait_recv()

            if step < planes - 1:
                onward, hop_copy = hop(step + 1, way)

                @pl.when(onward)
                def _(hop_copy=hop_copy):
                    hop_copy.start()

            @pl.when(valid)
            def _(block=block):
                select(block, held.at[block])

        if step == 1:
            pass_on(z)
        else:
            for way in range(2):
                valid, block, copy = arrival(step - 1, way)

                @pl.when(valid)
                def _(block=block):
                    pass_on(block)

    if planes == 1:
        pass_on(z)
    else:
        for way in range(2):
            valid, block, copy = arrival(planes - 1, way)

            @pl.when(valid)
            def _(block=block):
                pass_on(block)

    for copy in table_copies:
        copy.wait_send()
    for step in range(1, planes):
        for way in range(2):
            valid, copy = hop(step, way)

            @pl.when(valid)
            def _(copy=copy):
                copy.wait_send()

    def drain(block, carry):
        def one(d, inner):
            for part in range(2):
                pair_copy(block, d, part).wait()

                @pl.when(d > 0)
                def _():
                    plane_copy(block, d, part, q, (q + d) % width).wait_send()

            return inner

        return lax.fori_loop(0, width, one, carry)

    lax.fori_loop(0, planes, drain, 0)


def dispatch(planes, x, table, cap):
    experts_count, rows = table.shape[1:]
    width = experts_count // planes
    model = x.shape[1]
    vmem = pl.BlockSpec(memory_space=pltpu.VMEM)
    anywhere = pl.BlockSpec(memory_space=pl.ANY)
    landed = jax.ShapeDtypeStruct((planes, width, cap, model), BF16)
    far = max(planes - 1, 1)
    return pl.pallas_call(
        functools.partial(dispatch_kernel, planes, width, cap),
        out_shape=(landed, landed, jax.ShapeDtypeStruct((planes,) + table.shape, F32)),
        in_specs=[vmem, vmem],
        out_specs=(anywhere, anywhere, vmem),
        scratch_shapes=[
            pltpu.VMEM((planes, rows, model), BF16),
            pltpu.VMEM((planes, width, cap, model), BF16),
            pltpu.SemaphoreType.DMA((2, far)),
            pltpu.SemaphoreType.DMA((2, far, 2)),
            pltpu.SemaphoreType.DMA((2, planes, width, 2)),
            pltpu.SemaphoreType.DMA((planes, 2)),
            pltpu.SemaphoreType.DMA((2, planes, width, 2)),
        ],
        compiler_params=pltpu.CompilerParams(
            has_side_effects=True, vmem_limit_bytes=60 * 2**20
        ),
        name="dispatch",
    )(x, table)


def local(planes, tokens, expert_ids, gates, cotangent, w_gate, w_up, w_down, sh_gate, sh_up, sh_down):
    experts_count = lax.axis_size("ep")
    width = experts_count // planes
    me, core = lax.axis_index("ep"), lax.axis_index("tp")
    z, q = me // width, me % width
    tok_rows, model_width = tokens.shape
    top_count = expert_ids.shape[1]
    capacity = 3 * tok_rows * top_count // (2 * experts_count)
    half_cols = model_width // lax.axis_size("tp")
    first_col = core * half_cols

    lanes = jnp.arange(experts_count, dtype=jnp.int32)
    earlier = jnp.tril(jnp.ones((tok_rows, tok_rows), BF16), -1)

    def ranks_of(names):
        rank = jnp.dot(earlier, names.astype(BF16), preferred_element_type=F32)
        return jnp.where(names, rank.astype(jnp.int32), -1)

    mine = expert_ids[:, :, None] == lanes
    rank = ranks_of(jnp.any(mine, axis=1))
    gate_of = jnp.sum(jnp.where(mine, gates[:, :, None], 0.0), axis=1)
    slots = jnp.arange(capacity, dtype=jnp.int32)
    picked = rank.T[:, None, :] == slots[None, :, None]
    table = jnp.stack([rank.T.astype(F32), gate_of.T])
    x = jnp.concatenate(
        [
            lax.dynamic_slice_in_dim(tokens, first_col, half_cols, 1),
            lax.dynamic_slice_in_dim(cotangent, first_col, half_cols, 1),
        ],
        axis=1,
    )
    got_in, got_cot, line_table = dispatch(planes, x, table, capacity)
    got_in = got_in.reshape(experts_count * capacity, model_width)
    got_cot = got_cot.reshape(experts_count * capacity, model_width)
    shared_g, shared_u, shared_d, shared_part, unused = expert_backward(
        tokens, cotangent, sh_gate, sh_up, sh_down
    )
    grad_g, grad_u, grad_d, routed_part, gate_part = expert_backward(
        got_in, got_cot, w_gate[0], w_up[0], w_down[0]
    )

    part_rows = model_width // experts_count
    hidden_cols = sh_gate.shape[1]
    pieces = hidden_cols // part_rows
    deal = (planes, width, part_rows, hidden_cols)
    down = shared_d.astype(BF16).reshape(pieces, part_rows, experts_count, part_rows)
    down = down.transpose(2, 1, 0, 3).reshape(deal)
    grads = jnp.concatenate(
        [shared_g.astype(BF16).reshape(deal), shared_u.astype(BF16).reshape(deal), down], axis=2
    )

    senders = z * width + (q - jnp.arange(width, dtype=jnp.int32)) % width
    line_rank = line_table[:, 0][:, senders]
    scatter = (line_rank[..., None] == slots.astype(F32)).astype(BF16)

    def halves(values):
        return (
            lax.dynamic_slice_in_dim(values, first_col, half_cols, 1),
            lax.dynamic_slice_in_dim(values, half_cols - first_col, half_cols, 1),
        )

    own, oth = halves(routed_part)
    sh_own, sh_oth = halves(shared_part)
    blocks = (planes, width, capacity, half_cols)
    token_grad, shared_sum = combine(
        planes, own.reshape(blocks), oth.reshape(blocks), sh_own, sh_oth, scatter, grads
    )
    out_g = shared_sum[:part_rows]
    out_u = shared_sum[part_rows : 2 * part_rows]
    out_d = (
        shared_sum[2 * part_rows :]
        .reshape(part_rows, pieces, part_rows)
        .transpose(1, 0, 2)
        .reshape(hidden_cols, part_rows)
    )

    down_part = jnp.sum(out_d * out_d, axis=1)
    small = jnp.concatenate(
        [
            gate_part.reshape(experts_count, capacity),
            jnp.broadcast_to(down_part, (experts_count, hidden_cols)),
        ],
        axis=1,
    )
    small = lax.all_to_all(small, "ep", split_axis=0, concat_axis=0, tiled=True)
    back_gate, gate_norms, up_norms, shared_gate_norms, shared_up_norms = lax.psum(
        (
            small[:, :capacity],
            jnp.sum(grad_g * grad_g, axis=1),
            jnp.sum(grad_u * grad_u, axis=1),
            jnp.sum(out_g * out_g, axis=1),
            jnp.sum(out_u * out_u, axis=1),
        ),
        "tp",
    )
    down_norms = jnp.sum(small[:, capacity:], axis=0)
    token_gate = jnp.sum(jnp.where(picked, back_gate[:, :, None], 0.0), axis=1)
    gate_grad = jnp.sum(jnp.where(mine, token_gate.T[:, None, :], 0.0), axis=2) / gates
    return (
        token_grad,
        gate_grad,
        grad_g[None],
        grad_u[None],
        grad_d[None],
        out_g,
        out_u,
        out_d,
        gate_norms[None],
        up_norms[None],
        jnp.sum(grad_d * grad_d, axis=1)[None],
        shared_gate_norms,
        shared_up_norms,
        down_norms,
    )


def solution(mesh):
    placed = (
        P("ep", None),
        P("ep", None),
        P("ep", None),
        P("ep", None),
        P("ep", None, "tp"),
        P("ep", None, "tp"),
        P("ep", "tp", None),
        P(None, "tp"),
        P(None, "tp"),
        P("tp", None),
    )
    return jax.shard_map(
        functools.partial(local, plane_count(mesh)),
        mesh=mesh,
        in_specs=placed,
        out_specs=(
            P("ep", "tp"),
            P("ep", None),
            P("ep", None, "tp"),
            P("ep", None, "tp"),
            P("ep", "tp", None),
            P("ep", "tp"),
            P("ep", "tp"),
            P("tp", "ep"),
            P("ep", None),
            P("ep", None),
            P("ep", "tp"),
            P("ep"),
            P("ep"),
            P("tp"),
        ),
        check_vma=False,
    )
```

```python
import functools
import math

import jax
import jax.numpy as jnp
from jax import lax
from jax.experimental import pallas as pl
from jax.experimental.pallas import tpu as pltpu
from jax.sharding import PartitionSpec as P

BF16 = jnp.bfloat16
F32 = jnp.float32


def silu_parts(pre):
    sigmoid = jax.nn.sigmoid(pre)
    return (pre * sigmoid, sigmoid * (1.0 + pre * (1.0 - sigmoid)))


def expert_backward(inputs, cot_rows, w_g, w_u, w_d):
    gate_pre = jnp.dot(inputs, w_g, preferred_element_type=F32)
    up_pre = jnp.dot(inputs, w_u, preferred_element_type=F32)
    active, slope = silu_parts(gate_pre)
    hidden = (active * up_pre).astype(BF16)
    hidden_cot = jnp.dot(cot_rows, w_d.T, preferred_element_type=F32)
    gate_part = jnp.sum(hidden.astype(F32) * hidden_cot, axis=1)
    d_gate = (hidden_cot * up_pre * slope).astype(BF16)
    d_up = (hidden_cot * active).astype(BF16)
    contract = (((0,), (0,)), ((), ()))
    grad_g = lax.dot_general(inputs, d_gate, contract, preferred_element_type=F32)
    grad_u = lax.dot_general(inputs, d_up, contract, preferred_element_type=F32)
    grad_d = lax.dot_general(hidden, cot_rows, contract, preferred_element_type=F32)
    partial_value = jnp.dot(d_gate, w_g.T, preferred_element_type=F32) + jnp.dot(
        d_up, w_u.T, preferred_element_type=F32
    )
    return (grad_g, grad_u, grad_d, partial_value.astype(BF16), gate_part)


def plane_count(mesh):
    count = mesh.shape["ep"]
    try:
        planes = len({tuple(d.coords)[2] for d in mesh.devices.flat})
    except (AttributeError, TypeError, IndexError):
        planes = 0
    if planes < 1 or count % planes:
        planes = max(d for d in range(1, math.isqrt(count) + 1) if count % d == 0)
    return planes


def copy_to(src, dst, send, recv, ep, tp):
    return pltpu.make_async_remote_copy(
        src_ref=src,
        dst_ref=dst,
        send_sem=send,
        recv_sem=recv,
        device_id=(ep, tp),
        device_id_type=pl.DeviceIdType.MESH,
    )


def combine_kernel(
    planes, width,
    own, oth, sh_own, sh_oth, scatter, grads,
    tok_out, grad_out,
    tp_in, sh_in, sums, plane_in, gplane_in, z_out, z_in, gz_out, gz_in, routed, gtotal,
    tp_sem, plane_sem, gplane_sem, z_sem, gz_sem,
):
    me, core = lax.axis_index("ep"), lax.axis_index("tp")
    z, q = me // width, me % width
    order = list(range(1, planes)) + [0]
    dest_z = [(z + step) % planes for step in order]
    dest_q = [(q + step) % width for step in range(width)]
    started = []

    def start(copy):
        copy.start()
        started.append(copy)
        return copy

    tp_copies = [
        start(copy_to(oth.at[dest_z[i]], tp_in.at[i], tp_sem.at[0, i], tp_sem.at[1, i], me, 1 - core))
        for i in range(planes)
    ]
    sh_copy = start(
        copy_to(sh_oth, sh_in, tp_sem.at[0, planes], tp_sem.at[1, planes], me, 1 - core)
    )
    plane_copies, gplane_copies = {}, {}
    for i in range(planes):
        for d in range(1, width):
            peer = z * width + dest_q[d]
            gplane_copies[i, d] = start(
                copy_to(
                    grads.at[dest_z[i], dest_q[d]],
                    gplane_in.at[i, d - 1],
                    gplane_sem.at[0, i, d - 1],
                    gplane_sem.at[1, i, d - 1],
                    peer,
                    core,
                )
            )
        tp_copies[i].wait_recv()
        for d in range(width):
            sums[i, d] = (
                own[dest_z[i], dest_q[d]].astype(F32) + tp_in[i, dest_q[d]].astype(F32)
            ).astype(BF16)
            if d:
                peer = z * width + dest_q[d]
                plane_copies[i, d] = start(
                    copy_to(
                        sums.at[i, d],
                        plane_in.at[i, d - 1],
                        plane_sem.at[0, i, d - 1],
                        plane_sem.at[1, i, d - 1],
                        peer,
                        core,
                    )
                )
    z_copies = []
    for i in range(planes):
        peer = dest_z[i] * width + q
        total = grads[dest_z[i], q].astype(F32)
        for d in range(1, width):
            gplane_copies[i, d].wait_recv()
            total = total + gplane_in[i, d - 1].astype(F32)
        if i < planes - 1:
            gz_out[i] = total.astype(BF16)
            z_copies.append(
                start(copy_to(gz_out.at[i], gz_in.at[i], gz_sem.at[0, i], gz_sem.at[1, i], peer, core))
            )
        else:
            gtotal[...] = total
        for d in range(1, width):
            plane_copies[i, d].wait_recv()
        acc = jnp.dot(scatter[dest_z[i], 0], sums[i, 0], preferred_element_type=F32)
        for d in range(1, width):
            acc = acc + jnp.dot(
                scatter[dest_z[i], d], plane_in[i, d - 1], preferred_element_type=F32
            )
        if i < planes - 1:
            z_out[i] = acc.astype(BF16)
            z_copies.append(
                start(copy_to(z_out.at[i], z_in.at[i], z_sem.at[0, i], z_sem.at[1, i], peer, core))
            )
        else:
            routed[...] = acc
    sh_copy.wait_recv()
    for copy in z_copies:
        copy.wait_recv()
    total = gtotal[...]
    acc = routed[...]
    for i in range(planes - 1):
        total = total + gz_in[i].astype(F32)
        acc = acc + z_in[i].astype(F32)
    grad_out[...] = total
    acc = acc + (sh_own[...].astype(F32) + sh_in[...].astype(F32))
    tok_out[...] = acc.astype(BF16)
    for copy in started:
        copy.wait_send()


def combine(planes, own, oth, sh_own, sh_oth, scatter, grads):
    width = own.shape[1]
    cap, cols = own.shape[2:]
    rows = sh_own.shape[0]
    g_shape = grads.shape[2:]
    vmem = pl.BlockSpec(memory_space=pltpu.VMEM)
    far, side = max(planes - 1, 1), max(width - 1, 1)
    return pl.pallas_call(
        functools.partial(combine_kernel, planes, width),
        out_shape=(
            jax.ShapeDtypeStruct((rows, cols), BF16),
            jax.ShapeDtypeStruct(g_shape, F32),
        ),
        in_specs=[vmem] * 6,
        out_specs=(vmem, vmem),
        scratch_shapes=[
            pltpu.VMEM((planes, width, cap, cols), BF16),
            pltpu.VMEM((rows, cols), BF16),
            pltpu.VMEM((planes, width, cap, cols), BF16),
            pltpu.VMEM((planes, side, cap, cols), BF16),
            pltpu.VMEM((planes, side) + g_shape, BF16),
            pltpu.VMEM((far, rows, cols), BF16),
            pltpu.VMEM((far, rows, cols), BF16),
            pltpu.VMEM((far,) + g_shape, BF16),
            pltpu.VMEM((far,) + g_shape, BF16),
            pltpu.VMEM((rows, cols), F32),
            pltpu.VMEM(g_shape, F32),
            pltpu.SemaphoreType.DMA((2, planes + 1)),
            pltpu.SemaphoreType.DMA((2, planes, side)),
            pltpu.SemaphoreType.DMA((2, planes, side)),
            pltpu.SemaphoreType.DMA((2, far)),
            pltpu.SemaphoreType.DMA((2, far)),
        ],
        compiler_params=pltpu.CompilerParams(
            has_side_effects=True, vmem_limit_bytes=60 * 2**20
        ),
        name="combine",
    )(own, oth, sh_own, sh_oth, scatter, grads)


def dispatch_kernel(
    planes, width, cap,
    x, table, tokens, cotangent, w_g, w_u, w_d,
    tok_out, cot_out, line_table, grads, sh_part,
    held, ready,
    table_sem, line_sem, plane_sem, own_sem, pair_sem,
):
    me, core = lax.axis_index("ep"), lax.axis_index("tp")
    z, q = me // width, me % width
    cols = x.shape[1] // 2
    mine = pl.ds(pl.multiple_of(core * cols, cols), cols)
    outs = (tok_out, cot_out)

    table_copies = []
    for step in range(1, planes):
        peer = (z + step) % planes * width + q
        copy = copy_to(
            table, line_table.at[z], table_sem.at[0, step - 1], table_sem.at[1, step - 1], peer, core
        )
        copy.start()
        table_copies.append(copy)
    line_table[z] = table[...]

    def hop(step, way):
        block = z - (step - 1) if way == 0 else z + (step - 1)
        there = z + 1 if way == 0 else z - 1
        valid = (block >= 0) & (block < planes) & (there >= 0) & (there < planes)
        block, there = jnp.clip(block, 0, planes - 1), jnp.clip(there, 0, planes - 1)
        source = x if step == 1 else held.at[block]
        copy = copy_to(
            source,
            held.at[block],
            line_sem.at[0, step - 1, way],
            line_sem.at[1, step - 1, way],
            there * width + q,
            core,
        )
        return valid, copy

    def arrival(step, way):
        block = z - step if way == 0 else z + step
        valid = (block >= 0) & (block < planes)
        block = jnp.clip(block, 0, planes - 1)
        copy = copy_to(
            held.at[block],
            held.at[block],
            line_sem.at[0, step - 1, way],
            line_sem.at[1, step - 1, way],
            me,
            1 - core,
        )
        return valid, block, copy

    def send_step(step):
        for way in range(2):
            valid, copy = hop(step, way)

            @pl.when(valid)
            def _(copy=copy):
                copy.start()

    def plane_copy(block, d, part, from_q, to_q):
        return copy_to(
            ready.at[block, d, :, pl.ds(part * cols, cols)],
            outs[part].at[block, from_q, :, mine],
            plane_sem.at[0, block, d, part],
            plane_sem.at[1, block, d, part],
            z * width + to_q,
            core,
        )

    def own_copy(block, part):
        return pltpu.make_async_copy(
            ready.at[block, 0, :, pl.ds(part * cols, cols)],
            outs[part].at[block, q, :, mine],
            own_sem.at[block, part],
        )

    def pair_copy(block, d, part):
        from_q = (q + width - d) % width
        return copy_to(
            outs[part].at[block, from_q, :, mine],
            outs[part].at[block, from_q, :, mine],
            pair_sem.at[0, block, d, part],
            pair_sem.at[1, block, d, part],
            me,
            1 - core,
        )

    def select(block, source):
        def one(index, carry):
            d = (index + 1) % width
            to_q = (q + d) % width
            expert = z * width + to_q
            ranks = line_table[block, 0, pl.ds(expert, 1), :]
            gates = line_table[block, 1, pl.ds(expert, 1), :]
            slots = lax.broadcasted_iota(jnp.int32, (cap, ranks.shape[1]), 0).astype(F32)
            hit = slots == ranks
            gate = jnp.sum(jnp.where(hit, gates, 0.0), axis=1, keepdims=True)
            rows = jnp.dot(
                jnp.where(hit, 1.0, 0.0).astype(BF16), source[...], preferred_element_type=F32
            )
            ready[block, d, :, :cols] = rows[:, :cols].astype(BF16)
            ready[block, d, :, cols:] = (rows[:, cols:] * gate).astype(BF16)

            @pl.when(d > 0)
            def _():
                for part in range(2):
                    plane_copy(block, d, part, q, to_q).start()

            @pl.when(d == 0)
            def _():
                for part in range(2):
                    own_copy(block, part).start()

            return carry

        lax.fori_loop(0, width, one, 0)

    def pass_on(block):
        for part in range(2):
            own_copy(block, part).wait()
            pair_copy(block, 0, part).start()

        def one(d, carry):
            for part in range(2):
                plane_copy(block, d, part, (q + width - d) % width, (q + d) % width).wait_recv()
                pair_copy(block, d, part).start()
            return carry

        lax.fori_loop(1, width, one, 0)

    def shared_expert():
        gate_pre = jnp.dot(tokens[...], w_g[...], preferred_element_type=F32)
        up_pre = jnp.dot(tokens[...], w_u[...], preferred_element_type=F32)
        active, slope = silu_parts(gate_pre)
        hidden = (active * up_pre).astype(BF16)
        last, first = (((1,), (1,)), ((), ())), (((0,), (0,)), ((), ()))
        hidden_cot = lax.dot_general(cotangent[...], w_d[...], last, preferred_element_type=F32)
        d_gate = (hidden_cot * up_pre * slope).astype(BF16)
        d_up = (hidden_cot * active).astype(BF16)
        part_rows = grads.shape[2] // 3
        pieces = grads.shape[3] // part_rows
        block = max(part_rows, 128)

        def one(index, carry):
            at = pl.ds(pl.multiple_of(index * block, block), block)
            rows = lax.dot_general(d_gate, w_g[at, :], last, preferred_element_type=F32)
            rows = rows + lax.dot_general(d_up, w_u[at, :], last, preferred_element_type=F32)
            sh_part[:, at] = rows.astype(BF16)
            toks = tokens[:, at]
            grad_g = lax.dot_general(toks, d_gate, first, preferred_element_type=F32).astype(BF16)
            grad_u = lax.dot_general(toks, d_up, first, preferred_element_type=F32).astype(BF16)
            grad_d = lax.dot_general(
                hidden, cotangent[:, at], first, preferred_element_type=F32
            ).astype(BF16)
            for i in range(block // part_rows):
                owner = index * (block // part_rows) + i
                oz, oq = owner // width, owner % width
                take = slice(i * part_rows, (i + 1) * part_rows)
                grads[oz, oq, :part_rows, :] = grad_g[take, :]
                grads[oz, oq, part_rows : 2 * part_rows, :] = grad_u[take, :]
                for p in range(pieces):
                    here = slice(p * part_rows, (p + 1) * part_rows)
                    grads[oz, oq, 2 * part_rows :, here] = grad_d[here, take]
            return carry

        lax.fori_loop(0, tokens.shape[1] // block, one, 0)

    send_step(1)
    select(z, x)
    shared_expert()
    for copy in table_copies:
        copy.wait_recv()
    for step in range(1, planes):
        for way in range(2):
            valid, block, copy = arrival(step, way)

            @pl.when(valid)
            def _(copy=copy):
                copy.wait_recv()

            if step < planes - 1:
                onward, hop_copy = hop(step + 1, way)

                @pl.when(onward)
                def _(hop_copy=hop_copy):
                    hop_copy.start()

            @pl.when(valid)
            def _(block=block):
                select(block, held.at[block])

        if step == 1:
            pass_on(z)
        else:
            for way in range(2):
                valid, block, copy = arrival(step - 1, way)

                @pl.when(valid)
                def _(block=block):
                    pass_on(block)

    if planes == 1:
        pass_on(z)
    else:
        for way in range(2):
            valid, block, copy = arrival(planes - 1, way)

            @pl.when(valid)
            def _(block=block):
                pass_on(block)

    for copy in table_copies:
        copy.wait_send()
    for step in range(1, planes):
        for way in range(2):
            valid, copy = hop(step, way)

            @pl.when(valid)
            def _(copy=copy):
                copy.wait_send()

    def drain(block, carry):
        def one(d, inner):
            for part in range(2):
                pair_copy(block, d, part).wait()

                @pl.when(d > 0)
                def _():
                    plane_copy(block, d, part, q, (q + d) % width).wait_send()

            return inner

        return lax.fori_loop(0, width, one, carry)

    lax.fori_loop(0, planes, drain, 0)


def dispatch(planes, x, table, cap, shared):
    experts_count, rows = table.shape[1:]
    width = experts_count // planes
    model = x.shape[1]
    vmem = pl.BlockSpec(memory_space=pltpu.VMEM)
    anywhere = pl.BlockSpec(memory_space=pl.ANY)
    landed = jax.ShapeDtypeStruct((planes, width, cap, model), BF16)
    far = max(planes - 1, 1)
    hidden_cols = shared[2].shape[1]
    deal = (planes, width, 3 * (model // experts_count), hidden_cols)
    return pl.pallas_call(
        functools.partial(dispatch_kernel, planes, width, cap),
        out_shape=(
            landed,
            landed,
            jax.ShapeDtypeStruct((planes,) + table.shape, F32),
            jax.ShapeDtypeStruct(deal, BF16),
            jax.ShapeDtypeStruct((rows, model), BF16),
        ),
        in_specs=[vmem] * 7,
        out_specs=(anywhere, anywhere, vmem, vmem, vmem),
        scratch_shapes=[
            pltpu.VMEM((planes, rows, model), BF16),
            pltpu.VMEM((planes, width, cap, model), BF16),
            pltpu.SemaphoreType.DMA((2, far)),
            pltpu.SemaphoreType.DMA((2, far, 2)),
            pltpu.SemaphoreType.DMA((2, planes, width, 2)),
            pltpu.SemaphoreType.DMA((planes, 2)),
            pltpu.SemaphoreType.DMA((2, planes, width, 2)),
        ],
        compiler_params=pltpu.CompilerParams(
            has_side_effects=True, vmem_limit_bytes=60 * 2**20
        ),
        name="dispatch",
    )(x, table, *shared)


def local(planes, tokens, expert_ids, gates, cotangent, w_gate, w_up, w_down, sh_gate, sh_up, sh_down):
    experts_count = lax.axis_size("ep")
    width = experts_count // planes
    me, core = lax.axis_index("ep"), lax.axis_index("tp")
    z, q = me // width, me % width
    tok_rows, model_width = tokens.shape
    top_count = expert_ids.shape[1]
    capacity = 3 * tok_rows * top_count // (2 * experts_count)
    half_cols = model_width // lax.axis_size("tp")
    first_col = core * half_cols

    lanes = jnp.arange(experts_count, dtype=jnp.int32)
    earlier = jnp.tril(jnp.ones((tok_rows, tok_rows), BF16), -1)

    def ranks_of(names):
        rank = jnp.dot(earlier, names.astype(BF16), preferred_element_type=F32)
        return jnp.where(names, rank.astype(jnp.int32), -1)

    mine = expert_ids[:, :, None] == lanes
    rank = ranks_of(jnp.any(mine, axis=1))
    gate_of = jnp.sum(jnp.where(mine, gates[:, :, None], 0.0), axis=1)
    slots = jnp.arange(capacity, dtype=jnp.int32)
    picked = rank.T[:, None, :] == slots[None, :, None]
    table = jnp.stack([rank.T.astype(F32), gate_of.T])
    x = jnp.concatenate(
        [
            lax.dynamic_slice_in_dim(tokens, first_col, half_cols, 1),
            lax.dynamic_slice_in_dim(cotangent, first_col, half_cols, 1),
        ],
        axis=1,
    )
    shared = (tokens, cotangent, sh_gate, sh_up, sh_down)
    got_in, got_cot, line_table, grads, shared_part = dispatch(planes, x, table, capacity, shared)
    got_in = got_in.reshape(experts_count * capacity, model_width)
    got_cot = got_cot.reshape(experts_count * capacity, model_width)
    grad_g, grad_u, grad_d, routed_part, gate_part = expert_backward(
        got_in, got_cot, w_gate[0], w_up[0], w_down[0]
    )

    part_rows = model_width // experts_count
    hidden_cols = sh_gate.shape[1]
    pieces = hidden_cols // part_rows

    senders = z * width + (q - jnp.arange(width, dtype=jnp.int32)) % width
    line_rank = line_table[:, 0][:, senders]
    scatter = (line_rank[..., None] == slots.astype(F32)).astype(BF16)

    def halves(values):
        return (
            lax.dynamic_slice_in_dim(values, first_col, half_cols, 1),
            lax.dynamic_slice_in_dim(values, half_cols - first_col, half_cols, 1),
        )

    own, oth = halves(routed_part)
    sh_own, sh_oth = halves(shared_part)
    blocks = (planes, width, capacity, half_cols)
    token_grad, shared_sum = combine(
        planes, own.reshape(blocks), oth.reshape(blocks), sh_own, sh_oth, scatter, grads
    )
    out_g = shared_sum[:part_rows]
    out_u = shared_sum[part_rows : 2 * part_rows]
    out_d = (
        shared_sum[2 * part_rows :]
        .reshape(part_rows, pieces, part_rows)
        .transpose(1, 0, 2)
        .reshape(hidden_cols, part_rows)
    )

    down_part = jnp.sum(out_d * out_d, axis=1)
    small = jnp.concatenate(
        [
            gate_part.reshape(experts_count, capacity),
            jnp.broadcast_to(down_part, (experts_count, hidden_cols)),
        ],
        axis=1,
    )
    small = lax.all_to_all(small, "ep", split_axis=0, concat_axis=0, tiled=True)
    back_gate, gate_norms, up_norms, shared_gate_norms, shared_up_norms = lax.psum(
        (
            small[:, :capacity],
            jnp.sum(grad_g * grad_g, axis=1),
            jnp.sum(grad_u * grad_u, axis=1),
            jnp.sum(out_g * out_g, axis=1),
            jnp.sum(out_u * out_u, axis=1),
        ),
        "tp",
    )
    down_norms = jnp.sum(small[:, capacity:], axis=0)
    token_gate = jnp.sum(jnp.where(picked, back_gate[:, :, None], 0.0), axis=1)
    gate_grad = jnp.sum(jnp.where(mine, token_gate.T[:, None, :], 0.0), axis=2) / gates
    return (
        token_grad,
        gate_grad,
        grad_g[None],
        grad_u[None],
        grad_d[None],
        out_g,
        out_u,
        out_d,
        gate_norms[None],
        up_norms[None],
        jnp.sum(grad_d * grad_d, axis=1)[None],
        shared_gate_norms,
        shared_up_norms,
        down_norms,
    )


def solution(mesh):
    placed = (
        P("ep", None),
        P("ep", None),
        P("ep", None),
        P("ep", None),
        P("ep", None, "tp"),
        P("ep", None, "tp"),
        P("ep", "tp", None),
        P(None, "tp"),
        P(None, "tp"),
        P("tp", None),
    )
    return jax.shard_map(
        functools.partial(local, plane_count(mesh)),
        mesh=mesh,
        in_specs=placed,
        out_specs=(
            P("ep", "tp"),
            P("ep", None),
            P("ep", None, "tp"),
            P("ep", None, "tp"),
            P("ep", "tp", None),
            P("ep", "tp"),
            P("ep", "tp"),
            P("tp", "ep"),
            P("ep", None),
            P("ep", None),
            P("ep", "tp"),
            P("ep"),
            P("ep"),
            P("tp"),
        ),
        check_vma=False,
    )
```

```python
import functools
import math

import jax
import jax.numpy as jnp
from jax import lax
from jax.experimental import pallas as pl
from jax.experimental.pallas import tpu as pltpu
from jax.sharding import PartitionSpec as P

BF16 = jnp.bfloat16
F32 = jnp.float32


def silu_parts(pre):
    sigmoid = jax.nn.sigmoid(pre)
    return (pre * sigmoid, sigmoid * (1.0 + pre * (1.0 - sigmoid)))


def expert_backward(inputs, cot_rows, w_g, w_u, w_d):
    gate_pre = jnp.dot(inputs, w_g, preferred_element_type=F32)
    up_pre = jnp.dot(inputs, w_u, preferred_element_type=F32)
    active, slope = silu_parts(gate_pre)
    hidden = (active * up_pre).astype(BF16)
    hidden_cot = jnp.dot(cot_rows, w_d.T, preferred_element_type=F32)
    gate_part = jnp.sum(hidden.astype(F32) * hidden_cot, axis=1)
    d_gate = (hidden_cot * up_pre * slope).astype(BF16)
    d_up = (hidden_cot * active).astype(BF16)
    contract = (((0,), (0,)), ((), ()))
    grad_g = lax.dot_general(inputs, d_gate, contract, preferred_element_type=F32)
    grad_u = lax.dot_general(inputs, d_up, contract, preferred_element_type=F32)
    grad_d = lax.dot_general(hidden, cot_rows, contract, preferred_element_type=F32)
    partial_value = jnp.dot(d_gate, w_g.T, preferred_element_type=F32) + jnp.dot(
        d_up, w_u.T, preferred_element_type=F32
    )
    return (grad_g, grad_u, grad_d, partial_value.astype(BF16), gate_part)


def plane_count(mesh):
    count = mesh.shape["ep"]
    try:
        planes = len({tuple(d.coords)[2] for d in mesh.devices.flat})
    except (AttributeError, TypeError, IndexError):
        planes = 0
    if planes < 1 or count % planes:
        planes = max(d for d in range(1, math.isqrt(count) + 1) if count % d == 0)
    return planes


def copy_to(src, dst, send, recv, ep, tp):
    return pltpu.make_async_remote_copy(
        src_ref=src,
        dst_ref=dst,
        send_sem=send,
        recv_sem=recv,
        device_id=(ep, tp),
        device_id_type=pl.DeviceIdType.MESH,
    )


def combine_kernel(
    planes, width,
    parts, sh_parts, scatter, grads,
    tok_out, grad_out,
    tp_in, sh_in, sums, plane_in, gplane_in, z_out, z_in, gz_out, gz_in, routed, gtotal,
    tp_sem, plane_sem, gplane_sem, z_sem, gz_sem,
):
    me, core = lax.axis_index("ep"), lax.axis_index("tp")
    z, q = me // width, me % width
    cols = tok_out.shape[1]
    mine = pl.ds(pl.multiple_of(core * cols, cols), cols)
    other = pl.ds(pl.multiple_of((1 - core) * cols, cols), cols)
    order = list(range(1, planes)) + [0]
    dest_z = [(z + step) % planes for step in order]
    dest_q = [(q + step) % width for step in range(width)]
    started = []

    def start(copy):
        copy.start()
        started.append(copy)
        return copy

    tp_copies = [
        start(copy_to(parts.at[dest_z[i], :, :, other], tp_in.at[i], tp_sem.at[0, i], tp_sem.at[1, i], me, 1 - core))
        for i in range(planes)
    ]
    sh_copy = start(
        copy_to(sh_parts.at[:, other], sh_in, tp_sem.at[0, planes], tp_sem.at[1, planes], me, 1 - core)
    )
    plane_copies, gplane_copies = {}, {}
    for i in range(planes):
        for d in range(1, width):
            peer = z * width + dest_q[d]
            gplane_copies[i, d] = start(
                copy_to(
                    grads.at[dest_z[i], dest_q[d]],
                    gplane_in.at[i, d - 1],
                    gplane_sem.at[0, i, d - 1],
                    gplane_sem.at[1, i, d - 1],
                    peer,
                    core,
                )
            )
        tp_copies[i].wait_recv()
        for d in range(width):
            sums[i, d] = (
                parts[dest_z[i], dest_q[d], :, mine].astype(F32) + tp_in[i, dest_q[d]].astype(F32)
            ).astype(BF16)
            if d:
                peer = z * width + dest_q[d]
                plane_copies[i, d] = start(
                    copy_to(
                        sums.at[i, d],
                        plane_in.at[i, d - 1],
                        plane_sem.at[0, i, d - 1],
                        plane_sem.at[1, i, d - 1],
                        peer,
                        core,
                    )
                )
    z_copies = []
    for i in range(planes):
        peer = dest_z[i] * width + q
        total = grads[dest_z[i], q].astype(F32)
        for d in range(1, width):
            gplane_copies[i, d].wait_recv()
            total = total + gplane_in[i, d - 1].astype(F32)
        if i < planes - 1:
            gz_out[i] = total.astype(BF16)
            z_copies.append(
                start(copy_to(gz_out.at[i], gz_in.at[i], gz_sem.at[0, i], gz_sem.at[1, i], peer, core))
            )
        else:
            gtotal[...] = total
        for d in range(1, width):
            plane_copies[i, d].wait_recv()
        acc = jnp.dot(scatter[dest_z[i], 0], sums[i, 0], preferred_element_type=F32)
        for d in range(1, width):
            acc = acc + jnp.dot(
                scatter[dest_z[i], d], plane_in[i, d - 1], preferred_element_type=F32
            )
        if i < planes - 1:
            z_out[i] = acc.astype(BF16)
            z_copies.append(
                start(copy_to(z_out.at[i], z_in.at[i], z_sem.at[0, i], z_sem.at[1, i], peer, core))
            )
        else:
            routed[...] = acc
    sh_copy.wait_recv()
    for copy in z_copies:
        copy.wait_recv()
    total = gtotal[...]
    acc = routed[...]
    for i in range(planes - 1):
        total = total + gz_in[i].astype(F32)
        acc = acc + z_in[i].astype(F32)
    grad_out[...] = total
    acc = acc + (sh_parts[:, mine].astype(F32) + sh_in[...].astype(F32))
    tok_out[...] = acc.astype(BF16)
    for copy in started:
        copy.wait_send()


def combine(planes, cols, parts, sh_parts, scatter, grads):
    width, cap = parts.shape[1:3]
    rows = sh_parts.shape[0]
    g_shape = grads.shape[2:]
    vmem = pl.BlockSpec(memory_space=pltpu.VMEM)
    far, side = max(planes - 1, 1), max(width - 1, 1)
    return pl.pallas_call(
        functools.partial(combine_kernel, planes, width),
        out_shape=(
            jax.ShapeDtypeStruct((rows, cols), BF16),
            jax.ShapeDtypeStruct(g_shape, F32),
        ),
        in_specs=[vmem] * 4,
        out_specs=(vmem, vmem),
        scratch_shapes=[
            pltpu.VMEM((planes, width, cap, cols), BF16),
            pltpu.VMEM((rows, cols), BF16),
            pltpu.VMEM((planes, width, cap, cols), BF16),
            pltpu.VMEM((planes, side, cap, cols), BF16),
            pltpu.VMEM((planes, side) + g_shape, BF16),
            pltpu.VMEM((far, rows, cols), BF16),
            pltpu.VMEM((far, rows, cols), BF16),
            pltpu.VMEM((far,) + g_shape, BF16),
            pltpu.VMEM((far,) + g_shape, BF16),
            pltpu.VMEM((rows, cols), F32),
            pltpu.VMEM(g_shape, F32),
            pltpu.SemaphoreType.DMA((2, planes + 1)),
            pltpu.SemaphoreType.DMA((2, planes, side)),
            pltpu.SemaphoreType.DMA((2, planes, side)),
            pltpu.SemaphoreType.DMA((2, far)),
            pltpu.SemaphoreType.DMA((2, far)),
        ],
        compiler_params=pltpu.CompilerParams(
            has_side_effects=True, vmem_limit_bytes=40 * 2**20
        ),
        name="combine",
    )(parts, sh_parts, scatter, grads)


def dispatch_kernel(
    planes, width, cap,
    x, table, tokens, cotangent, w_g, w_u, w_d,
    tok_out, cot_out, line_table, grads, sh_part,
    held, ready,
    table_sem, line_sem, plane_sem, own_sem, pair_sem,
):
    me, core = lax.axis_index("ep"), lax.axis_index("tp")
    z, q = me // width, me % width
    cols = x.shape[1] // 2
    mine = pl.ds(pl.multiple_of(core * cols, cols), cols)
    outs = (tok_out, cot_out)

    table_copies = []
    for step in range(1, planes):
        peer = (z + step) % planes * width + q
        copy = copy_to(
            table, line_table.at[z], table_sem.at[0, step - 1], table_sem.at[1, step - 1], peer, core
        )
        copy.start()
        table_copies.append(copy)
    line_table[z] = table[...]

    def hop(step, way):
        block = z - (step - 1) if way == 0 else z + (step - 1)
        there = z + 1 if way == 0 else z - 1
        valid = (block >= 0) & (block < planes) & (there >= 0) & (there < planes)
        block, there = jnp.clip(block, 0, planes - 1), jnp.clip(there, 0, planes - 1)
        source = x if step == 1 else held.at[block]
        copy = copy_to(
            source,
            held.at[block],
            line_sem.at[0, step - 1, way],
            line_sem.at[1, step - 1, way],
            there * width + q,
            core,
        )
        return valid, copy

    def arrival(step, way):
        block = z - step if way == 0 else z + step
        valid = (block >= 0) & (block < planes)
        block = jnp.clip(block, 0, planes - 1)
        copy = copy_to(
            held.at[block],
            held.at[block],
            line_sem.at[0, step - 1, way],
            line_sem.at[1, step - 1, way],
            me,
            1 - core,
        )
        return valid, block, copy

    def send_step(step):
        for way in range(2):
            valid, copy = hop(step, way)

            @pl.when(valid)
            def _(copy=copy):
                copy.start()

    def plane_copy(block, d, part, from_q, to_q):
        return copy_to(
            ready.at[block, d, :, pl.ds(part * cols, cols)],
            outs[part].at[block, from_q, :, mine],
            plane_sem.at[0, block, d, part],
            plane_sem.at[1, block, d, part],
            z * width + to_q,
            core,
        )

    def own_copy(block, part):
        return pltpu.make_async_copy(
            ready.at[block, 0, :, pl.ds(part * cols, cols)],
            outs[part].at[block, q, :, mine],
            own_sem.at[block, part],
        )

    def pair_copy(block, d, part):
        from_q = (q + width - d) % width
        return copy_to(
            outs[part].at[block, from_q, :, mine],
            outs[part].at[block, from_q, :, mine],
            pair_sem.at[0, block, d, part],
            pair_sem.at[1, block, d, part],
            me,
            1 - core,
        )

    def select(block, source):
        def one(index, carry):
            d = (index + 1) % width
            to_q = (q + d) % width
            expert = z * width + to_q
            ranks = line_table[block, 0, pl.ds(expert, 1), :]
            gates = line_table[block, 1, pl.ds(expert, 1), :]
            slots = lax.broadcasted_iota(jnp.int32, (cap, ranks.shape[1]), 0).astype(F32)
            hit = slots == ranks
            gate = jnp.sum(jnp.where(hit, gates, 0.0), axis=1, keepdims=True)
            rows = jnp.dot(
                jnp.where(hit, 1.0, 0.0).astype(BF16), source[...], preferred_element_type=F32
            )
            ready[block, d, :, :cols] = rows[:, :cols].astype(BF16)
            ready[block, d, :, cols:] = (rows[:, cols:] * gate).astype(BF16)

            @pl.when(d > 0)
            def _():
                for part in range(2):
                    plane_copy(block, d, part, q, to_q).start()

            @pl.when(d == 0)
            def _():
                for part in range(2):
                    own_copy(block, part).start()

            return carry

        lax.fori_loop(0, width, one, 0)

    def pass_on(block):
        for part in range(2):
            own_copy(block, part).wait()
            pair_copy(block, 0, part).start()

        def one(d, carry):
            for part in range(2):
                plane_copy(block, d, part, (q + width - d) % width, (q + d) % width).wait_recv()
                pair_copy(block, d, part).start()
            return carry

        lax.fori_loop(1, width, one, 0)

    def shared_expert():
        gate_pre = jnp.dot(tokens[...], w_g[...], preferred_element_type=F32)
        up_pre = jnp.dot(tokens[...], w_u[...], preferred_element_type=F32)
        active, slope = silu_parts(gate_pre)
        hidden = (active * up_pre).astype(BF16)
        last, first = (((1,), (1,)), ((), ())), (((0,), (0,)), ((), ()))
        hidden_cot = lax.dot_general(cotangent[...], w_d[...], last, preferred_element_type=F32)
        d_gate = (hidden_cot * up_pre * slope).astype(BF16)
        d_up = (hidden_cot * active).astype(BF16)
        part_rows = grads.shape[2] // 3
        pieces = grads.shape[3] // part_rows
        block = max(part_rows, 128)

        def one(index, carry):
            at = pl.ds(pl.multiple_of(index * block, block), block)
            rows = lax.dot_general(d_gate, w_g[at, :], last, preferred_element_type=F32)
            rows = rows + lax.dot_general(d_up, w_u[at, :], last, preferred_element_type=F32)
            sh_part[:, at] = rows.astype(BF16)
            toks = tokens[:, at]
            grad_g = lax.dot_general(toks, d_gate, first, preferred_element_type=F32).astype(BF16)
            grad_u = lax.dot_general(toks, d_up, first, preferred_element_type=F32).astype(BF16)
            grad_d = lax.dot_general(
                hidden, cotangent[:, at], first, preferred_element_type=F32
            ).astype(BF16)
            for i in range(block // part_rows):
                owner = index * (block // part_rows) + i
                oz, oq = owner // width, owner % width
                take = slice(i * part_rows, (i + 1) * part_rows)
                grads[oz, oq, :part_rows, :] = grad_g[take, :]
                grads[oz, oq, part_rows : 2 * part_rows, :] = grad_u[take, :]
                for p in range(pieces):
                    here = slice(p * part_rows, (p + 1) * part_rows)
                    grads[oz, oq, 2 * part_rows :, here] = grad_d[here, take]
            return carry

        lax.fori_loop(0, tokens.shape[1] // block, one, 0)

    send_step(1)
    select(z, x)
    shared_expert()
    for copy in table_copies:
        copy.wait_recv()
    for step in range(1, planes):
        for way in range(2):
            valid, block, copy = arrival(step, way)

            @pl.when(valid)
            def _(copy=copy):
                copy.wait_recv()

            if step < planes - 1:
                onward, hop_copy = hop(step + 1, way)

                @pl.when(onward)
                def _(hop_copy=hop_copy):
                    hop_copy.start()

            @pl.when(valid)
            def _(block=block):
                select(block, held.at[block])

        if step == 1:
            pass_on(z)
        else:
            for way in range(2):
                valid, block, copy = arrival(step - 1, way)

                @pl.when(valid)
                def _(block=block):
                    pass_on(block)

    if planes == 1:
        pass_on(z)
    else:
        for way in range(2):
            valid, block, copy = arrival(planes - 1, way)

            @pl.when(valid)
            def _(block=block):
                pass_on(block)

    for copy in table_copies:
        copy.wait_send()
    for step in range(1, planes):
        for way in range(2):
            valid, copy = hop(step, way)

            @pl.when(valid)
            def _(copy=copy):
                copy.wait_send()

    def drain(block, carry):
        def one(d, inner):
            for part in range(2):
                pair_copy(block, d, part).wait()

                @pl.when(d > 0)
                def _():
                    plane_copy(block, d, part, q, (q + d) % width).wait_send()

            return inner

        return lax.fori_loop(0, width, one, carry)

    lax.fori_loop(0, planes, drain, 0)


def dispatch(planes, x, table, cap, shared):
    experts_count, rows = table.shape[1:]
    width = experts_count // planes
    model = x.shape[1]
    vmem = pl.BlockSpec(memory_space=pltpu.VMEM)
    anywhere = pl.BlockSpec(memory_space=pl.ANY)
    landed = jax.ShapeDtypeStruct((planes, width, cap, model), BF16)
    far = max(planes - 1, 1)
    hidden_cols = shared[2].shape[1]
    deal = (planes, width, 3 * (model // experts_count), hidden_cols)
    return pl.pallas_call(
        functools.partial(dispatch_kernel, planes, width, cap),
        out_shape=(
            landed,
            landed,
            jax.ShapeDtypeStruct((planes,) + table.shape, F32),
            jax.ShapeDtypeStruct(deal, BF16),
            jax.ShapeDtypeStruct((rows, model), BF16),
        ),
        in_specs=[vmem] * 7,
        out_specs=(anywhere, anywhere, vmem, vmem, vmem),
        scratch_shapes=[
            pltpu.VMEM((planes, rows, model), BF16),
            pltpu.VMEM((planes, width, cap, model), BF16),
            pltpu.SemaphoreType.DMA((2, far)),
            pltpu.SemaphoreType.DMA((2, far, 2)),
            pltpu.SemaphoreType.DMA((2, planes, width, 2)),
            pltpu.SemaphoreType.DMA((planes, 2)),
            pltpu.SemaphoreType.DMA((2, planes, width, 2)),
        ],
        compiler_params=pltpu.CompilerParams(
            has_side_effects=True, vmem_limit_bytes=40 * 2**20
        ),
        name="dispatch",
    )(x, table, *shared)


def local(planes, tokens, expert_ids, gates, cotangent, w_gate, w_up, w_down, sh_gate, sh_up, sh_down):
    experts_count = lax.axis_size("ep")
    width = experts_count // planes
    me, core = lax.axis_index("ep"), lax.axis_index("tp")
    z, q = me // width, me % width
    tok_rows, model_width = tokens.shape
    top_count = expert_ids.shape[1]
    capacity = 3 * tok_rows * top_count // (2 * experts_count)
    half_cols = model_width // lax.axis_size("tp")
    first_col = core * half_cols

    lanes = jnp.arange(experts_count, dtype=jnp.int32)
    earlier = jnp.tril(jnp.ones((tok_rows, tok_rows), BF16), -1)

    def ranks_of(names):
        rank = jnp.dot(earlier, names.astype(BF16), preferred_element_type=F32)
        return jnp.where(names, rank.astype(jnp.int32), -1)

    mine = expert_ids[:, :, None] == lanes
    rank = ranks_of(jnp.any(mine, axis=1))
    gate_of = jnp.sum(jnp.where(mine, gates[:, :, None], 0.0), axis=1)
    slots = jnp.arange(capacity, dtype=jnp.int32)
    picked = rank.T[:, None, :] == slots[None, :, None]
    table = jnp.stack([rank.T.astype(F32), gate_of.T])
    x = jnp.concatenate(
        [
            lax.dynamic_slice_in_dim(tokens, first_col, half_cols, 1),
            lax.dynamic_slice_in_dim(cotangent, first_col, half_cols, 1),
        ],
        axis=1,
    )
    shared = (tokens, cotangent, sh_gate, sh_up, sh_down)
    got_in, got_cot, line_table, grads, shared_part = dispatch(planes, x, table, capacity, shared)
    got_in = got_in.reshape(experts_count * capacity, model_width)
    got_cot = got_cot.reshape(experts_count * capacity, model_width)
    grad_g, grad_u, grad_d, routed_part, gate_part = expert_backward(
        got_in, got_cot, w_gate[0], w_up[0], w_down[0]
    )

    part_rows = model_width // experts_count
    hidden_cols = sh_gate.shape[1]
    pieces = hidden_cols // part_rows

    senders = z * width + (q - jnp.arange(width, dtype=jnp.int32)) % width
    line_rank = line_table[:, 0][:, senders]
    scatter = (line_rank[..., None] == slots.astype(F32)).astype(BF16)

    blocks = (planes, width, capacity, model_width)
    token_grad, shared_sum = combine(
        planes, half_cols, routed_part.reshape(blocks), shared_part, scatter, grads
    )
    out_g = shared_sum[:part_rows]
    out_u = shared_sum[part_rows : 2 * part_rows]
    out_d = (
        shared_sum[2 * part_rows :]
        .reshape(part_rows, pieces, part_rows)
        .transpose(1, 0, 2)
        .reshape(hidden_cols, part_rows)
    )

    down_part = jnp.sum(out_d * out_d, axis=1)
    small = jnp.concatenate(
        [
            gate_part.reshape(experts_count, capacity),
            jnp.broadcast_to(down_part, (experts_count, hidden_cols)),
        ],
        axis=1,
    )
    small = lax.all_to_all(small, "ep", split_axis=0, concat_axis=0, tiled=True)
    back_gate, gate_norms, up_norms, shared_gate_norms, shared_up_norms = lax.psum(
        (
            small[:, :capacity],
            jnp.sum(grad_g * grad_g, axis=1),
            jnp.sum(grad_u * grad_u, axis=1),
            jnp.sum(out_g * out_g, axis=1),
            jnp.sum(out_u * out_u, axis=1),
        ),
        "tp",
    )
    down_norms = jnp.sum(small[:, capacity:], axis=0)
    token_gate = jnp.sum(jnp.where(picked, back_gate[:, :, None], 0.0), axis=1)
    gate_grad = jnp.sum(jnp.where(mine, token_gate.T[:, None, :], 0.0), axis=2) / gates
    return (
        token_grad,
        gate_grad,
        grad_g[None],
        grad_u[None],
        grad_d[None],
        out_g,
        out_u,
        out_d,
        gate_norms[None],
        up_norms[None],
        jnp.sum(grad_d * grad_d, axis=1)[None],
        shared_gate_norms,
        shared_up_norms,
        down_norms,
    )


def solution(mesh):
    placed = (
        P("ep", None),
        P("ep", None),
        P("ep", None),
        P("ep", None),
        P("ep", None, "tp"),
        P("ep", None, "tp"),
        P("ep", "tp", None),
        P(None, "tp"),
        P(None, "tp"),
        P("tp", None),
    )
    return jax.shard_map(
        functools.partial(local, plane_count(mesh)),
        mesh=mesh,
        in_specs=placed,
        out_specs=(
            P("ep", "tp"),
            P("ep", None),
            P("ep", None, "tp"),
            P("ep", None, "tp"),
            P("ep", "tp", None),
            P("ep", "tp"),
            P("ep", "tp"),
            P("tp", "ep"),
            P("ep", None),
            P("ep", None),
            P("ep", "tp"),
            P("ep"),
            P("ep"),
            P("tp"),
        ),
        check_vma=False,
    )
```
